128 devices in a mesh: ep: 32 (over z, y, core), tp: 4 (over x).
Axes of the slice: x: 4, y: 4, z: 4, core: 2. Of those that a mesh axis runs over, the one named last changes fastest.
Arguments:
- hidden: bfloat16 [2048, 2048], P('ep'), may hold values from -10 to 10
- mix_gain: bfloat16 [2048], replicated, may hold values from 0.099609375 to 1.8984375
- proj_x: bfloat16 [2048, 2048], P('ep', 'tp'), may hold values from -0.125 to 0.125
- proj_y: bfloat16 [2048, 2048], P('ep', 'tp'), may hold values from -0.125 to 0.125
- conv_taps: bfloat16 [4, 2048], P(None, 'tp'), may hold values from -3 to 3
- input_gate: bfloat16 [32, 64, 64], P('tp'), may hold values from -0.75 to 0.75
- decay_gate: bfloat16 [32, 64, 64], P('tp'), may hold values from -0.75 to 0.75
- decay_param: float32 [2048], P('tp'), may hold values from 1 to 6
- proj_out: bfloat16 [2048, 2048], P('tp'), may hold values from -0.125 to 0.125
- conv_state: bfloat16 [2048, 3, 2048], P('ep', None, 'tp'), may hold values from -6 to 6
- lru_state: float32 [2048, 2048], P('ep', 'tp'), may hold values from -6 to 6
- ffn_gain: bfloat16 [2048], replicated, may hold values from 0.099609375 to 1.8984375
- routes: int32 [2048, 2], P('ep'), may hold values from 0 to 31, all different within a row; in each aligned block of 64 rows (0 to 63, 64 to 127, ...) at most 6 rows name the same one
- route_weights: float32 [2048, 2], P('ep'), may hold values from 0.2 to 1
- expert_gate: bfloat16 [32, 2048, 3072], P('ep', None, 'tp'), may hold values from -0.125 to 0.125
- expert_up: bfloat16 [32, 2048, 3072], P('ep', None, 'tp'), may hold values from -0.125 to 0.125
- expert_down: bfloat16 [32, 3072, 2048], P('ep', 'tp'), may hold values from -0.109375 to 0.109375
- dense_gate: bfloat16 [2048, 6144], P('tp', 'ep'), may hold values from -0.125 to 0.125
- dense_up: bfloat16 [2048, 6144], P('tp', 'ep'), may hold values from -0.125 to 0.125
- dense_down: bfloat16 [6144, 2048], P('ep', 'tp'), may hold values from -0.078125 to 0.078125
- branch_gate: float32 [2048], P('tp'), may hold values from -4 to 4
Outputs:
- new_hidden: bfloat16 [2048, 2048], P('ep', 'tp')
- new_lru: float32 [2048, 2048], P('ep', 'tp')
- new_conv: bfloat16 [2048, 3, 2048], P('ep', None, 'tp')
The draws below stay inside these ranges and needn't reach their ends.
Inputs may be any that keep to these rules, and one draw needn't show every extreme that they name: `routes`: each row names 2 different experts. In the 64 rows of one index of ep, no expert is named by more than 6 rows, a bound that some block reaches.
All inputs are finite; a program needn't handle non-finite values.
Results may differ from the reference program's by a relative error of at most 0.017.
Values may be sent and summed in bfloat16 or wider, within the bound.
A program may use at most 128 MiB of HBM per device.

```python
import math
import jax
import jax.numpy as jnp
import numpy as np
from jax import lax

D = 2048
HEADS = 32
BLOCK = 64
LRU = 2048
TAPS = 4
FFE = 3072
DFF = 6144
EXPERTS = 32
TOPK = 2
SEQ_DEV = 64
BATCH = 2048
CAP = 6
N_EP = 32
N_TP = 4


def draw_hidden(key, part):
    noise_key = jax.random.fold_in(key, 11)
    column = jnp.arange(D, dtype=jnp.float32) / (D - 1)
    scales = 0.5 * jnp.power(4.0, column)
    values = jax.random.normal(noise_key, (BATCH, D), jnp.float32) * scales[None, :]
    return jnp.clip(values, -10.0, 10.0).astype(jnp.bfloat16)


def shard_levels(rng, shape, cuts, smallest, top_value):
    loudness = 1.0
    for dim, shards_of in cuts:
        draws = jax.random.uniform(jax.random.fold_in(jax.random.fold_in(rng, 6), dim), (shards_of,), jnp.float32, smallest / len(cuts), top_value / len(cuts))
        loudness = loudness * jnp.repeat(jnp.exp(draws), shape[dim] // shards_of).reshape((-1,) + (1,) * (len(shape) - 1 - dim))
    return loudness


def assign_block(key, own, number, rows, count, top, reach, slope):
    sequence = jax.random.permutation(key, count)
    crowded, common = portions_of(count, rows * top, reach, slope, True), portions_of(count, rows * top, reach, slope, False)
    places = jnp.arange(count)

    def named(lengths, turn):
        used = int((lengths > 0).sum())
        fixed = max(1, used // 4)
        passed = fixed + (places - fixed + turn * (used - fixed)) % max(1, count - fixed)
        return jnp.zeros((count,), jnp.int32).at[sequence[jnp.where(places < fixed, places, passed)]].set(jnp.asarray(lengths, jnp.int32))

    lengths = jnp.where(number % 4 == 0, named(crowded, number // 4), named(common, number - number // 4 - 1))
    mixed = jax.random.permutation(jax.random.fold_in(own, 3), count)
    source_of, receiver = mixed[0:count // 2 * 2:2], mixed[1:count // 2 * 2:2]
    margin = jnp.minimum(lengths[source_of] - 1, reach - lengths[receiver]) // 2
    margin = jnp.where((source_of == sequence[0]) | (receiver == sequence[0]) | (lengths[receiver] == 0), 0, jnp.maximum(margin, 0))
    passed = jax.random.randint(jax.random.fold_in(own, 4), (count // 2,), 0, 1 << 20) % (margin + 1)
    lengths = lengths.at[source_of].add(-passed).at[receiver].add(passed)
    labels = jnp.searchsorted(jnp.cumsum(lengths), jnp.arange(rows * top), side="right").astype(jnp.int32)
    listing = labels.reshape(top, rows).T
    listing = listing[jax.random.permutation(jax.random.fold_in(own, 1), rows)]
    turn = jax.random.randint(jax.random.fold_in(own, 2), (rows, 1), 0, top)
    return jnp.take_along_axis(listing, (jnp.arange(top)[None, :] + turn) % top, axis=1)


def portions_of(count, total, limit, lean, full):
    portions = [(1 << 20) // math.isqrt(rank ** lean) + 1 for rank in range(1, count + 1)]
    largest = limit if full else min(limit, max(-(-total // count), total * portions[0] // sum(portions)))
    least = 1 if total - largest >= count - 1 else 0
    counts, rest = [largest] + [least] * (count - 1), total - largest - least * (count - 1)
    while rest > 0:
        movable = [i for i in range(1, count) if counts[i] < largest] or [i for i in range(1, count) if counts[i] < limit]
        whole, budget = sum([portions[i] for i in movable]), rest
        for i in movable:
            addition = min(limit - counts[i], max(1, budget * portions[i] // whole), rest)
            counts[i] = counts[i] + addition
            rest = rest - addition
    return np.array(counts)


def bell_draw(stream_key, dims, spread, reach, split=(), held_as=jnp.bfloat16):
    values = jax.random.normal(stream_key, dims, jnp.float32) * spread
    if len(split) > 0:
        values = shard_levels(stream_key, dims, split, -0.22, 0.18) * values
    return jnp.clip(values, min=-reach, max=reach).astype(held_as)


def setup_inputs(seed: int = 0) -> dict:
    streams_of = jax.random.split(jax.random.key(seed), 22)
    hidden = draw_hidden(jax.random.fold_in(streams_of[21], 71), 0)
    mix_gain = jnp.clip(1.0 + 0.18 * jax.random.normal(streams_of[1], (D,), jnp.float32), 0.099609375, 1.8984375).astype(jnp.bfloat16)
    proj_x = bell_draw(streams_of[2], (D, LRU), D ** -0.5, 0.125, ((0, 32), (1, 4)))
    proj_y = bell_draw(streams_of[3], (D, LRU), D ** -0.5, 0.125, ((0, 32), (1, 4)))
    conv_taps = bell_draw(streams_of[4], (TAPS, LRU), 0.5, 3.0, ((1, 4),))
    input_gate = bell_draw(streams_of[5], (HEADS, BLOCK, BLOCK), BLOCK ** -0.5, 0.75, ((0, 4),))
    decay_gate = bell_draw(streams_of[6], (HEADS, BLOCK, BLOCK), BLOCK ** -0.5, 0.75, ((0, 4),))
    decay_param = jnp.clip(1.0 + 5.0 * jax.random.uniform(streams_of[7], (LRU,), jnp.float32) ** shard_levels(streams_of[7], (LRU,), ((0, 4),), -0.2, 0.2), 1.0, 6.0)
    proj_out = bell_draw(streams_of[8], (LRU, D), LRU ** -0.5, 0.125, ((0, 4),))
    conv_state = bell_draw(streams_of[9], (BATCH, TAPS - 1, LRU), 1.0, 6.0, ((0, 32), (2, 4)))
    lru_state = bell_draw(streams_of[10], (BATCH, LRU), 1.0, 6.0, ((0, 32), (1, 4)), jnp.float32)
    ffn_gain = jnp.clip(1.0 + 0.18 * jax.random.normal(streams_of[11], (D,), jnp.float32), 0.099609375, 1.8984375).astype(jnp.bfloat16)
    routes_keys = jax.random.split(jax.random.fold_in(streams_of[12], 1), BATCH // SEQ_DEV)
    routes_turns = jax.random.permutation(jax.random.fold_in(streams_of[12], 3), BATCH // SEQ_DEV)
    routes = jax.vmap(lambda own, number: assign_block(jax.random.fold_in(streams_of[12], 2), own, number, SEQ_DEV, EXPERTS, TOPK, CAP, 1))(routes_keys, routes_turns).reshape((BATCH, TOPK))
    route_weights = jnp.clip(jnp.exp(math.log(1.0) - 1.609438 * jax.random.uniform(streams_of[13], (BATCH, TOPK), jnp.float32) ** shard_levels(streams_of[13], (BATCH, TOPK), ((0, 32),), -0.2, 0.2)), 0.2, 1.0)
    expert_gate = bell_draw(streams_of[14], (EXPERTS, D, FFE), D ** -0.5, 0.125, ((0, 32), (2, 4)))
    expert_up = bell_draw(streams_of[15], (EXPERTS, D, FFE), D ** -0.5, 0.125, ((0, 32), (2, 4)))
    expert_down = bell_draw(streams_of[16], (EXPERTS, FFE, D), FFE ** -0.5, 0.109375, ((0, 32), (1, 4)))
    dense_gate = bell_draw(streams_of[17], (D, DFF), D ** -0.5, 0.125, ((0, 4), (1, 32)))
    dense_up = bell_draw(streams_of[18], (D, DFF), D ** -0.5, 0.125, ((0, 4), (1, 32)))
    dense_down = bell_draw(streams_of[19], (DFF, D), DFF ** -0.5, 0.078125, ((0, 32), (1, 4)))
    branch_gate = bell_draw(streams_of[20], (D,), 1.0, 4.0, ((0, 4),), jnp.float32)
    return dict(hidden=hidden, mix_gain=mix_gain, proj_x=proj_x, proj_y=proj_y, conv_taps=conv_taps, input_gate=input_gate, decay_gate=decay_gate, decay_param=decay_param, proj_out=proj_out, conv_state=conv_state, lru_state=lru_state, ffn_gain=ffn_gain, routes=routes, route_weights=route_weights, expert_gate=expert_gate, expert_up=expert_up, expert_down=expert_down, dense_gate=dense_gate, dense_up=dense_up, dense_down=dense_down, branch_gate=branch_gate)


epsilon = 1e-06
decay_scale = 8.0

def rms_scale(values, gain_vec):
    floats = values.astype(jnp.float32)
    meansq = lax.optimization_barrier(jnp.mean(floats * floats, axis=-1, keepdims=True))
    return floats * lax.rsqrt(meansq + epsilon) * gain_vec.astype(jnp.float32)

def reference(hidden, mix_gain, proj_x, proj_y, conv_taps, input_gate, decay_gate, decay_param, proj_out, conv_state, lru_state, ffn_gain, routes, route_weights, expert_gate, expert_up, expert_down, dense_gate, dense_up, dense_down, branch_gate):
    batch_rows = hidden.shape[0]
    lru_width = HEADS * BLOCK
    normed = rms_scale(hidden, mix_gain).astype(jnp.bfloat16)
    x_proj = jnp.dot(normed, proj_x, preferred_element_type=jnp.float32).astype(jnp.bfloat16)
    y_proj = jnp.dot(normed, proj_y, preferred_element_type=jnp.float32).astype(jnp.bfloat16)
    window = jnp.concatenate([conv_state, x_proj[:, None, :]], axis=1)
    conv_out = lax.optimization_barrier(jnp.sum(window.astype(jnp.float32) * conv_taps.astype(jnp.float32)[None], axis=1)).astype(jnp.bfloat16)
    heads_in = conv_out.astype(jnp.float32).reshape(batch_rows, HEADS, BLOCK)
    gate_in = jax.nn.sigmoid(jnp.einsum('bhi,hij->bhj', heads_in, input_gate.astype(jnp.float32)).reshape(batch_rows, lru_width))
    gate_dec = jax.nn.sigmoid(jnp.einsum('bhi,hij->bhj', heads_in, decay_gate.astype(jnp.float32)).reshape(batch_rows, lru_width))
    log_decay = decay_scale * gate_dec * jax.nn.log_sigmoid(decay_param)
    decay_rate = jnp.exp(log_decay)
    inject = jnp.sqrt(-jnp.expm1(2.0 * log_decay))
    new_lru = decay_rate * lru_state + inject * gate_in * conv_out.astype(jnp.float32)
    gated_out = (new_lru * jax.nn.gelu(y_proj.astype(jnp.float32))).astype(jnp.bfloat16)
    head_share = lru_width // N_TP
    mixer_sum = jnp.zeros((batch_rows, D), jnp.float32)
    for member in range(N_TP):
        partial_value = jnp.dot(gated_out[:, member * head_share:(member + 1) * head_share], proj_out[member * head_share:(member + 1) * head_share], preferred_element_type=jnp.float32).astype(jnp.bfloat16)
        mixer_sum = mixer_sum + partial_value.astype(jnp.float32)
    summed = (hidden.astype(jnp.float32) + mixer_sum).astype(jnp.bfloat16)
    ffn_in = rms_scale(summed, ffn_gain).astype(jnp.bfloat16)
    pair_expert = routes.reshape(-1).astype(jnp.int32)
    onehot = (pair_expert[:, None] == jnp.arange(EXPERTS, dtype=jnp.int32)[None, :]).astype(jnp.int32)
    grouped = onehot.reshape(N_EP, SEQ_DEV * TOPK, EXPERTS)
    before = jnp.cumsum(grouped, axis=1) - grouped
    slot_rank = lax.optimization_barrier(jnp.sum(before * grouped, axis=2)).reshape(-1)
    group_of = jnp.arange(BATCH * TOPK, dtype=jnp.int32) // (SEQ_DEV * TOPK)
    position = (group_of * CAP + slot_rank).astype(jnp.int32)
    token_of = jnp.arange(BATCH * TOPK, dtype=jnp.int32) // TOPK
    buffer = jnp.zeros((EXPERTS, N_EP * CAP, D), jnp.bfloat16).at[pair_expert, position].set(ffn_in[token_of])
    ff_share = FFE // N_TP

    def one_expert(operands):
        slot_rows, gate_w, up_w, down_w = operands
        gate_val = jnp.dot(slot_rows, gate_w, preferred_element_type=jnp.float32)
        up_val = jnp.dot(slot_rows, up_w, preferred_element_type=jnp.float32)
        inner_act = (jax.nn.silu(gate_val) * up_val).astype(jnp.bfloat16)
        total_out = jnp.zeros((slot_rows.shape[0], D), jnp.float32)
        for member in range(N_TP):
            piece_out = jnp.dot(inner_act[:, member * ff_share:(member + 1) * ff_share], down_w[member * ff_share:(member + 1) * ff_share], preferred_element_type=jnp.float32).astype(jnp.bfloat16)
            total_out = total_out + piece_out.astype(jnp.float32)
        return total_out.astype(jnp.bfloat16)
    results = lax.map(one_expert, (buffer, expert_gate, expert_up, expert_down))
    picked = results[pair_expert, position].astype(jnp.float32)
    expert_sum = lax.optimization_barrier(jnp.sum((picked * route_weights.reshape(-1)[:, None]).reshape(batch_rows, TOPK, D), axis=1))
    dense_g = jnp.dot(ffn_in, dense_gate, preferred_element_type=jnp.float32)
    dense_u = jnp.dot(ffn_in, dense_up, preferred_element_type=jnp.float32)
    dense_hid = (jax.nn.silu(dense_g) * dense_u).astype(jnp.bfloat16)
    dense_out = jnp.dot(dense_hid, dense_down, preferred_element_type=jnp.float32)
    new_hidden = (summed.astype(jnp.float32) + expert_sum + jax.nn.sigmoid(branch_gate)[None, :] * dense_out).astype(jnp.bfloat16)
    return (new_hidden, new_lru, window[:, 1:])
```

```python
import jax
import jax.numpy as jnp
from jax import lax
from jax.experimental import pallas as pl
from jax.experimental.pallas import tpu as pltpu
from jax.sharding import PartitionSpec as P

MESH = pl.DeviceIdType.MESH
F32 = jnp.float32
BF16 = jnp.bfloat16
I32 = jnp.int32

epsilon = 1e-06
decay_scale = 8.0
D = 2048
COLS = 512
OFFS = (0, -1, 1, 2)


def dot(a, b):
    return jnp.dot(a, b, preferred_element_type=F32)


def dot_nt(a, b):
    return lax.dot_general(a, b, (((1,), (1,)), ((), ())), preferred_element_type=F32)


def iota(shape, dim):
    return lax.broadcasted_iota(I32, shape, dim)


def mask(cond):
    return jnp.where(cond, 1.0, 0.0)


def div6(v):
    return (v * 171) >> 10


def rms_scale(floats, gain):
    meansq = jnp.mean(floats * floats, axis=-1, keepdims=True)
    return floats * lax.rsqrt(meansq + epsilon) * gain.astype(F32)


def sigmoid(v):
    return 1.0 / (1.0 + jnp.exp(-v))


def neg_expm1(v):
    series = -v * (1.0 + v * (1 / 2) * (1.0 + v * (1 / 3) * (1.0 + v * (1 / 4) * (1.0 + v * (1 / 5)))))
    return jnp.where(v > -0.1, series, 1.0 - jnp.exp(v))


def kernel(
    mix_gain, conv_taps, input_gate, decay_gate, decay_param, ffn_gain, routes, route_weights,
    branch_gate, hidden_h, proj_x_h, proj_y_h, proj_out_h, conv_h, lru_h, eg_h, eu_h, ed_h,
    dg_h, du_h, dd_h,
    new_hidden, new_lru, x_out,
    hid, px, py, wo, conv, lru, eg, eu, ed, dg, du, dd,
    gx, gy, wown, wgu, wd, nrm, bd_in, bd_dec, csum, gout, pp, rsb, smb, sxb, xall, dtok,
    fstack, sel, comb, perm, qmat, disp, arr, xrows, inner, pe, er, ret, back,
    dhid, dpart, drecv, dsb, dxb,
    lsem, ag_s, ag_r, dw_s, dw_r, rs_s, rs_r, xa_s, xa_r, sm_s, sm_r, da_s, da_r,
    di_s, di_r, er_s, er_r, re_s, re_r, dr_s, dr_r, dx_s, dx_r,
):
    ep = lax.axis_index("ep")
    x = lax.axis_index("tp")
    c = lax.rem(ep, 2)
    chip = lax.div(ep, 2)
    y = lax.rem(chip, 4)
    z = lax.div(chip, 4)

    def m4(v):
        return lax.rem(v + 8, 4)

    def cp(src, dst, ssem, rsem, dev):
        return pltpu.make_async_remote_copy(
            src_ref=src, dst_ref=dst, send_sem=ssem, recv_sem=rsem, device_id=dev, device_id_type=MESH
        )

    loads = [
        (proj_x_h, px), (proj_y_h, py), (hidden_h, hid), (dg_h, dg), (du_h, du), (dd_h, dd),
        (conv_h, conv), (lru_h, lru), (proj_out_h, wo), (eg_h.at[0], eg), (eu_h.at[0], eu),
        (ed_h.at[0], ed),
    ]

    def load(k):
        return pltpu.make_async_copy(loads[k][0], loads[k][1], lsem.at[k])

    for k in range(len(loads)):
        load(k).start()

    bar = pltpu.get_barrier_semaphore()

    def greet(k, carry):
        pl.semaphore_signal(bar, inc=1, device_id=(lax.rem(ep + k, 32), x), device_id_type=MESH)
        return carry

    lax.fori_loop(1, 32, greet, 0)
    for k in (1, 2, 3):
        pl.semaphore_signal(bar, inc=1, device_id=(ep, m4(x + k)), device_id_type=MESH)
    load(0).wait()
    load(1).wait()
    pl.semaphore_wait(bar, 34)

    own = (px, py)
    bufs = (gx, gy)
    first = (y, z)
    second = (z, y)

    def chip_of(h, f, s):
        return (s * 4 + f) if h == 0 else (f * 4 + s)

    def slot(h, f, s, cc):
        return bufs[h].at[s, f, cc] if h == 0 else bufs[h].at[f, s, cc]

    def piece(h, f, s, half):
        return slot(h, f, s, c).at[pl.ds(32 * half, 32), :]

    def dev(h, f, s, cc):
        return (chip_of(h, f, s) * 2 + cc, x)

    sent = []

    def go(copy):
        copy.start()
        sent.append(copy)

    def to_f(h, step, idx, src, dst):
        go(cp(src, dst, ag_s.at[h, idx], ag_r.at[h, idx], dev(h, m4(first[h] + step), second[h], c)))

    def to_s(h, step, idx, src, dst):
        go(cp(src, dst, ag_s.at[h, idx], ag_r.at[h, idx], dev(h, first[h], m4(second[h] + step), c)))

    def to_p(h, idx, src, dst):
        go(cp(src, dst, ag_s.at[h, idx], ag_r.at[h, idx], (chip * 2 + 1 - c, x)))

    def got(h, idx, dst):
        cp(dst, dst, ag_s.at[h, idx], ag_r.at[h, idx], (chip * 2 + 1 - c, x)).wait_recv()

    def second_phase(h, i, src):
        f, s = m4(first[h] + OFFS[i]), second[h]
        to_s(h, 1, 4 + 4 * i, src, slot(h, f, s, c))
        to_s(h, -1, 5 + 4 * i, src, slot(h, f, s, c))

    def across(h, i, si, src=None):
        f, s = m4(first[h] + OFFS[i]), m4(second[h] + OFFS[si])
        mine = slot(h, f, s, c)
        to_p(h, 20 + 4 * si + i, mine if src is None else src, mine)

    for h in range(2):
        f, s = first[h], second[h]
        to_f(h, 1, 0, own[h], slot(h, f, s, c))
        to_f(h, -1, 1, own[h], slot(h, f, s, c))
    for h in range(2):
        second_phase(h, 0, own[h])
        across(h, 0, 0, own[h])
    gx[z, y, c] = px[...]
    gy[z, y, c] = py[...]

    r64 = iota((64, 128), 0)
    c128 = iota((64, 128), 1)
    put = (mask(c128 == r64).astype(BF16), mask(c128 == r64 + 64).astype(BF16))

    load(3).wait()
    load(4).wait()
    load(5).wait()
    wown[:, 0:128] = dg[:, 0:128]
    wown[:, 128:256] = du[:, 0:128]
    wown[:, 256:384] = (dot(dg[:, 128:192], put[0]) + dot(du[:, 128:192], put[1])).astype(BF16)

    load(2).wait()
    nrm[...] = rms_scale(hid[...].astype(F32), mix_gain[...]).astype(BF16)

    wsrc = (wown, dd)
    wdst = (wgu, wd)
    wrows = (256, 96)

    def w_go(a, idx, src, dst, device):
        go(cp(src, dst, dw_s.at[a, idx], dw_r.at[a, idx], device))

    def w_got(a, idx, dst):
        cp(dst, dst, dw_s.at[a, idx], dw_r.at[a, idx], (chip * 2 + 1 - c, x)).wait_recv()

    for a in range(2):
        w_go(a, 0, wsrc[a], wdst[a].at[c, x], (ep, m4(x + 1)))
        w_go(a, 1, wsrc[a], wdst[a].at[c, x], (ep, m4(x - 1)))
        w_go(a, 4, wsrc[a], wdst[a].at[c, x], (chip * 2 + 1 - c, x))
    wgu[c, x] = wown[...]
    wd[c, x] = dd[...]

    for h in range(2):
        f, s = first[h], second[h]
        lo, hi = m4(f - 1), m4(f + 1)
        got(h, 0, slot(h, lo, s, c))
        to_f(h, 1, 2, piece(h, lo, s, 0), piece(h, lo, s, 0))
        second_phase(h, 1, slot(h, lo, s, c))
        across(h, 1, 0)
        got(h, 1, slot(h, hi, s, c))
        to_f(h, -1, 3, piece(h, hi, s, 1), piece(h, hi, s, 1))
        second_phase(h, 2, slot(h, hi, s, c))
        across(h, 2, 0)

    def arrivals(h, i):
        f, s = m4(first[h] + OFFS[i]), second[h]
        lo, hi = m4(s - 1), m4(s + 1)
        got(h, 4 + 4 * i, slot(h, f, lo, c))
        to_s(h, 1, 6 + 4 * i, piece(h, f, lo, 0), piece(h, f, lo, 0))
        across(h, i, 1)
        got(h, 5 + 4 * i, slot(h, f, hi, c))
        to_s(h, -1, 7 + 4 * i, piece(h, f, hi, 1), piece(h, f, hi, 1))
        across(h, i, 2)

    def last(h, i):
        f, s = m4(first[h] + OFFS[i]), m4(second[h] + 2)
        got(h, 6 + 4 * i, piece(h, f, s, 0))
        got(h, 7 + 4 * i, piece(h, f, s, 1))
        across(h, i, 3)

    e32 = iota((64, 32), 1)
    oh = [mask(routes[:, r:r + 1] == e32) for r in range(2)]
    both = oh[0] + oh[1]
    lower = mask(iota((64, 64), 1) < iota((64, 64), 0)).astype(BF16)
    rank1 = both * (dot(lower, both.astype(BF16)) + 1.0)
    rank1b = rank1.astype(BF16)

    for h in range(2):
        arrivals(h, 0)
    for h in range(2):
        f, s = m4(first[h] + 2), second[h]
        got(h, 2, piece(h, f, s, 0))
        got(h, 3, piece(h, f, s, 1))
        second_phase(h, 3, slot(h, f, s, c))
        across(h, 3, 0)

    for p in range(4):
        for gate, block in ((input_gate, bd_in), (decay_gate, bd_dec)):
            for k in range(2):
                block[p, 64 * k:64 * k + 64, :] = dot(gate[2 * p + k], put[k]).astype(BF16)

    for h in range(2):
        arrivals(h, 1)

    load(6).wait()
    taps = conv_taps[...].astype(F32)
    csum[...] = jnp.sum(conv[...].astype(F32) * taps[None, 0:3, :], axis=1)

    for h in range(2):
        arrivals(h, 2)

    tt = mask((iota((512, 64), 0) & 63) == iota((512, 64), 1)).astype(BF16)
    spread = dot(tt, rank1b).astype(BF16)
    rows = iota((1536, 32), 0)
    ecol = iota((1536, 32), 1) * 48
    erow = mask((rows >= ecol) & (rows < ecol + 48)).astype(BF16)
    row1 = iota((1536, 1), 0)
    six1 = div6(row1 >> 3)
    rin = row1 - six1 * 48
    ck1 = div6(rin)
    slot1 = (rin - 6 * ck1 + 1).astype(F32)
    ckcol = iota((1536, 512), 1) >> 6
    sel[...] = mask((dot_nt(erow, spread) == slot1) & (ck1 == ckcol)).astype(BF16)

    for h in range(2):
        last(h, 0)
    for h in range(2):
        arrivals(h, 3)

    pr = iota((384, 384), 0)
    pc = iota((384, 384), 1)
    prc = div6(pr >> 3)
    prr = pr - 48 * prc
    prs = div6(prr)
    perm[...] = mask(pc == prs * 48 + prc * 6 + (prr - 6 * prs)).astype(BF16)
    qr = iota((512, 384), 0)
    qc = iota((512, 384), 1)
    qslot = qr & 7
    qmat[...] = mask((qslot < 6) & (qc == ((qr >> 3) & 1) * 192 + (qr >> 4) * 6 + qslot)).astype(BF16)

    for h in range(2):
        last(h, 1)

    w0 = route_weights[:, 0:1]
    w1 = route_weights[:, 1:2]
    wfull = w0 * oh[0] + w1 * oh[1]
    whi = wfull.astype(BF16)
    wlo = (wfull - whi.astype(F32)).astype(BF16)
    expand = mask((iota((32, 512), 1) >> 4) == iota((32, 512), 0)).astype(BF16)
    ccol = iota((64, 512), 1)
    hit = dot(rank1b, expand) == ((ccol & 7) + 1).astype(F32)
    ehi = dot(whi, expand)
    elo = dot(wlo, expand)
    for j in range(2):
        here = hit & (((ccol >> 3) & 1) == j)
        comb[j, 0] = jnp.where(here, ehi, 0.0).astype(BF16)
        comb[j, 1] = jnp.where(here, elo, 0.0).astype(BF16)

    for h in range(2):
        last(h, 2)
    for h in range(2):
        last(h, 3)

    for h in range(2):
        for si in range(4):
            for i in range(4):
                f, s = m4(first[h] + OFFS[i]), m4(second[h] + OFFS[si])
                got(h, 20 + 4 * si + i, slot(h, f, s, 1 - c))

    x_total = dot(nrm[:, 0:512], gx[0].reshape(512, 512))
    y_total = dot(nrm[:, 0:512], gy[0].reshape(512, 512))
    for k in range(1, 4):
        x_total += dot(nrm[:, 512 * k:512 * k + 512], gx[k].reshape(512, 512))
        y_total += dot(nrm[:, 512 * k:512 * k + 512], gy[k].reshape(512, 512))
    x_proj = x_total.astype(BF16)
    x_out[...] = x_proj
    conv_out = (csum[...] + x_proj.astype(F32) * taps[3:4, :]).astype(BF16)
    load(7).wait()
    for p in range(4):
        lanes = slice(128 * p, 128 * p + 128)
        co = conv_out[:, lanes]
        gate_in = sigmoid(dot(co, bd_in[p]))
        gate_dec = sigmoid(dot(co, bd_dec[p]))
        log_sig = -jnp.log(1.0 + jnp.exp(-decay_param[:, lanes]))
        log_decay = decay_scale * gate_dec * log_sig
        inject = jnp.sqrt(neg_expm1(2.0 * log_decay))
        state = jnp.exp(log_decay) * lru[:, lanes] + inject * gate_in * co.astype(F32)
        new_lru[:, lanes] = state
        yv = y_total[:, lanes].astype(BF16).astype(F32)
        gout[:, lanes] = (state * jax.nn.gelu(yv, approximate=True)).astype(BF16)

    load(8).wait()
    for k in range(4):
        lanes = slice(512 * k, 512 * k + 512)
        pp[:, :, lanes] = dot(gout[...], wo[:, lanes]).reshape(4, 16, 512).astype(BF16)

    def rs(k):
        to = m4(x + k)
        return cp(pp.at[to], rsb.at[x], rs_s.at[k], rs_r.at[k], (ep, to))

    for k in (2, 1, 3):
        go(rs(k))

    for a in range(2):
        lo, hi, r = m4(x - 1), m4(x + 1), wrows[a]
        w_got(a, 0, wdst[a].at[c, lo])
        part = wdst[a].at[c, lo, pl.ds(0, r), :]
        w_go(a, 2, part, part, (ep, hi))
        w_go(a, 5, wdst[a].at[c, lo], wdst[a].at[c, lo], (chip * 2 + 1 - c, x))
        w_got(a, 1, wdst[a].at[c, hi])
        part = wdst[a].at[c, hi, pl.ds(r, r), :]
        w_go(a, 3, part, part, (ep, lo))
        w_go(a, 6, wdst[a].at[c, hi], wdst[a].at[c, hi], (chip * 2 + 1 - c, x))

    mixed = pp[x].astype(F32)
    for k in (1, 3, 2):
        frm = m4(x - k)
        cp(rsb.at[frm], rsb.at[frm], rs_s.at[k], rs_r.at[k], (ep, frm)).wait_recv()
        mixed += rsb[frm].astype(F32)
    summed = (hid[pl.ds(pl.multiple_of(16 * x, 16), 16), :].astype(F32) + mixed).astype(BF16)
    for k in range(4):
        smb[k] = summed[:, 512 * k:512 * k + 512]
    xall[x] = rms_scale(summed.astype(F32), ffn_gain[...]).astype(BF16)
    dtok[chip] = xall[x]

    for k in (2, 1, 3):
        to = m4(x + k)
        go(cp(xall.at[x], xall.at[x], xa_s.at[k], xa_r.at[k], (ep, to)))

    def tok(k):
        to = lax.rem(chip + k, 16)
        return cp(xall.at[x], dtok.at[chip], da_s.at[k], da_r.at[k], (to * 2 + c, x))

    def each(first_k, end_k, act):
        def step(k, carry):
            act(k)
            return carry
        lax.fori_loop(first_k, end_k, step, 0)

    each(1, 16, lambda k: tok(k).start())
    for k in (2, 1, 3):
        to = m4(x + k)
        go(cp(smb.at[to], sxb.at[x], sm_s.at[k], sm_r.at[k], (ep, to)))
    sxb[x] = smb[x]

    for k in (1, 3, 2):
        frm = m4(x - k)
        cp(xall.at[frm], xall.at[frm], xa_s.at[k], xa_r.at[k], (ep, frm)).wait_recv()
    for k in range(8):
        fstack[64 * k:64 * k + 64, :] = xall[:, :, 256 * k:256 * k + 256].reshape(64, 256)
    for k in range(4):
        part = slice(384 * k, 384 * k + 384)
        disp[8 * k:8 * k + 8] = dot(sel[part, :], fstack[...]).reshape(8, 48, 256).astype(BF16)
    arr[ep] = disp[ep]

    def route(k):
        to = lax.rem(ep + k, 32)
        return cp(disp.at[to], arr.at[ep], di_s.at[k], di_r.at[k], (to, x))

    each(1, 32, lambda k: route(k).start())

    for a in range(2):
        far = m4(x + 2)
        r = wrows[a]
        w_got(a, 2, wdst[a].at[c, far, pl.ds(0, r), :])
        w_got(a, 3, wdst[a].at[c, far, pl.ds(r, r), :])
        w_go(a, 7, wdst[a].at[c, far], wdst[a].at[c, far], (chip * 2 + 1 - c, x))
    for a in range(2):
        for idx, off in ((4, 0), (5, -1), (6, 1), (7, 2)):
            w_got(a, idx, wdst[a].at[1 - c, m4(x + off)])

    def tok_got(k):
        frm = lax.rem(chip + 16 - k, 16)
        cp(dtok.at[frm], dtok.at[frm], da_s.at[k], da_r.at[k], (frm * 2 + c, x)).wait_recv()

    each(1, 16, tok_got)
    for cc in range(2):
        gu = dot(dtok[:, :, 0:512].reshape(256, 512), wgu[cc, 0])
        for k in range(1, 4):
            gu += dot(dtok[:, :, 512 * k:512 * k + 512].reshape(256, 512), wgu[cc, k])
        g0, u0, t2 = gu[:, 0:128], gu[:, 128:256], gu[:, 256:384]
        dhid[cc, :, 0:128] = (g0 * sigmoid(g0) * u0).astype(BF16)
        dhid[cc, :, 128:256] = (t2 * sigmoid(t2) * pltpu.roll(t2, 64, 1)).astype(BF16)
    for k in range(4):
        out = dot(dhid[0, :, 0:192], wd[0, k]) + dot(dhid[1, :, 0:192], wd[1, k])
        dpart[:, :, 512 * k:512 * k + 512] = out.reshape(16, 16, 512).astype(BF16)

    def dred(k):
        to = lax.rem(chip + k, 16)
        return cp(dpart.at[to], drecv.at[chip], dr_s.at[k], dr_r.at[k], (to * 2 + c, x))

    each(1, 16, lambda k: dred(k).start())
    drecv[chip] = dpart[chip]

    def route_got(k):
        frm = lax.rem(ep + 32 - k, 32)
        cp(arr.at[frm], arr.at[frm], di_s.at[k], di_r.at[k], (frm, x)).wait_recv()

    each(1, 32, route_got)
    for k in range(4):
        moved = dot(perm[...], arr[8 * k:8 * k + 8].reshape(384, 256)).astype(BF16)
        for j in range(8):
            xrows[48 * k:48 * k + 48, 256 * j:256 * j + 256] = moved[48 * j:48 * j + 48, :]
    load(9).wait()
    load(10).wait()
    for k in range(3):
        lanes = slice(256 * k, 256 * k + 256)
        gv = dot(xrows[...], eg[:, lanes])
        uv = dot(xrows[...], eu[:, lanes])
        inner[:, lanes] = (gv * sigmoid(gv) * uv).astype(BF16)
    load(11).wait()
    for k in (2, 1, 3, 0):
        to = m4(x + k)
        pe[to] = dot(inner[...], ed[:, pl.ds(pl.multiple_of(512 * to, 512), 512)]).astype(BF16)
        if k:
            go(cp(pe.at[to], er.at[x], er_s.at[k], er_r.at[k], (ep, to)))

    def dred_got(k):
        frm = lax.rem(chip + 16 - k, 16)
        cp(drecv.at[frm], drecv.at[frm], dr_s.at[k], dr_r.at[k], (frm * 2 + c, x)).wait_recv()

    each(1, 16, dred_got)
    for k in range(4):
        dsb[k] = jnp.sum(drecv[:, :, 512 * k:512 * k + 512].astype(F32), axis=0).astype(BF16)
    for k in (2, 1, 3):
        to = m4(x + k)
        go(cp(dsb.at[to], dxb.at[x], dx_s.at[k], dx_r.at[k], (ep, to)))
    dxb[x] = dsb[x]

    total = pe[x].astype(F32)
    for k in (1, 3, 2):
        frm = m4(x - k)
        cp(er.at[frm], er.at[frm], er_s.at[k], er_r.at[k], (ep, frm)).wait_recv()
        total += er[frm].astype(F32)
    total = total.astype(BF16)
    ret[...] = (
        dot(qmat[:, 0:192], total[:, 0:256]) + dot(qmat[:, 192:384], total[:, 256:512])
    ).reshape(32, 16, 256).astype(BF16)
    back[ep] = ret[ep]

    def giveback(k):
        to = lax.rem(ep + k, 32)
        return cp(ret.at[to], back.at[ep], re_s.at[k], re_r.at[k], (to, x))

    each(1, 32, lambda k: giveback(k).start())

    for k in (1, 3, 2):
        frm = m4(x - k)
        cp(sxb.at[frm], sxb.at[frm], sm_s.at[k], sm_r.at[k], (ep, frm)).wait_recv()
        cp(dxb.at[frm], dxb.at[frm], dx_s.at[k], dx_r.at[k], (ep, frm)).wait_recv()
    share = sigmoid(branch_gate[...])
    rest = sxb[...].reshape(64, 512).astype(F32) + share * dxb[...].reshape(64, 512).astype(F32)

    def back_got(k):
        frm = lax.rem(ep + 32 - k, 32)
        cp(back.at[frm], back.at[frm], re_s.at[k], re_r.at[k], (frm, x)).wait_recv()

    each(1, 32, back_got)
    rows_back = back[...].reshape(512, 256)
    for j in range(2):
        lanes = slice(256 * j, 256 * j + 256)
        esum = dot(comb[j, 0], rows_back) + dot(comb[j, 1], rows_back)
        new_hidden[:, lanes] = (rest[:, lanes] + esum).astype(BF16)

    for copy in sent:
        copy.wait_send()
    each(1, 16, lambda k: tok(k).wait_send())
    each(1, 16, lambda k: dred(k).wait_send())
    each(1, 32, lambda k: route(k).wait_send())
    each(1, 32, lambda k: giveback(k).wait_send())


def on_device(
    hidden, mix_gain, proj_x, proj_y, conv_taps, input_gate, decay_gate, decay_param, proj_out,
    conv_state, lru_state, ffn_gain, routes, route_weights, expert_gate, expert_up, expert_down,
    dense_gate, dense_up, dense_down, branch_gate,
):
    vmem = pl.BlockSpec(memory_space=pltpu.VMEM)
    hbm = pl.BlockSpec(memory_space=pl.ANY)
    V = pltpu.VMEM
    dma = pltpu.SemaphoreType.DMA
    scratch = [
        V((64, D), BF16), V((64, COLS), BF16), V((64, COLS), BF16), V((COLS, D), BF16),
        V((64, 3, COLS), BF16), V((64, COLS), F32), V((D, 768), BF16), V((D, 768), BF16),
        V((768, D), BF16), V((COLS, 192), BF16), V((COLS, 192), BF16), V((192, COLS), BF16),
        V((4, 4, 2, 64, COLS), BF16), V((4, 4, 2, 64, COLS), BF16), V((COLS, 384), BF16),
        V((2, 4, COLS, 384), BF16), V((2, 4, 192, COLS), BF16), V((64, D), BF16),
        V((4, 128, 128), BF16), V((4, 128, 128), BF16), V((64, COLS), F32), V((64, COLS), BF16),
        V((4, 16, D), BF16), V((4, 16, D), BF16), V((4, 16, COLS), BF16), V((4, 16, COLS), BF16),
        V((4, 16, D), BF16), V((16, 16, D), BF16),
        V((512, 256), BF16), V((1536, 512), BF16), V((2, 2, 64, 512), BF16), V((384, 384), BF16),
        V((512, 384), BF16), V((32, 48, 256), BF16), V((32, 48, 256), BF16), V((192, D), BF16),
        V((192, 768), BF16), V((4, 192, COLS), BF16), V((4, 192, COLS), BF16),
        V((32, 16, 256), BF16), V((32, 16, 256), BF16),
        V((2, 256, 256), BF16), V((16, 16, D), BF16), V((16, 16, D), BF16),
        V((4, 16, COLS), BF16), V((4, 16, COLS), BF16),
        dma((12,)), dma((2, 36)), dma((2, 36)), dma((2, 8)), dma((2, 8)), dma((4,)), dma((4,)),
        dma((4,)), dma((4,)), dma((4,)), dma((4,)), dma((16,)), dma((16,)), dma((32,)), dma((32,)),
        dma((4,)), dma((4,)), dma((32,)), dma((32,)), dma((16,)), dma((16,)), dma((4,)), dma((4,)),
    ]
    new_hidden, new_lru, x_proj = pl.pallas_call(
        kernel,
        out_shape=(
            jax.ShapeDtypeStruct((64, COLS), BF16),
            jax.ShapeDtypeStruct((64, COLS), F32),
            jax.ShapeDtypeStruct((64, COLS), BF16),
        ),
        in_specs=[vmem] * 9 + [hbm] * 12,
        out_specs=(vmem, vmem, vmem),
        scratch_shapes=scratch,
        compiler_params=pltpu.CompilerParams(
            collective_id=0, has_side_effects=True, vmem_limit_bytes=58 * 1024 * 1024
        ),
        name="decode_layer",
    )(
        mix_gain.reshape(1, D), conv_taps, input_gate, decay_gate, decay_param.reshape(1, COLS),
        ffn_gain.reshape(1, D), routes, route_weights, branch_gate.reshape(1, COLS),
        hidden, proj_x, proj_y, proj_out, conv_state, lru_state, expert_gate, expert_up,
        expert_down, dense_gate, dense_up, dense_down,
    )
    new_conv = jnp.concatenate([conv_state[:, 1:], x_proj[:, None, :]], axis=1)
    return (new_hidden, new_lru, new_conv)


def solution(mesh):
    in_specs = (
        P("ep", None), P(), P("ep", "tp"), P("ep", "tp"), P(None, "tp"), P("tp", None, None),
        P("tp", None, None), P("tp"), P("tp", None), P("ep", None, "tp"), P("ep", "tp"), P(),
        P("ep", None), P("ep", None), P("ep", None, "tp"), P("ep", None, "tp"),
        P("ep", "tp", None), P("tp", "ep"), P("tp", "ep"), P("ep", "tp"), P("tp"),
    )
    out_specs = (P("ep", "tp"), P("ep", "tp"), P("ep", None, "tp"))
    return jax.shard_map(
        on_device, mesh=mesh, in_specs=in_specs, out_specs=out_specs, check_vma=False
    )
```

```python
import jax
import jax.numpy as jnp
from jax import lax
from jax.experimental import pallas as pl
from jax.experimental.pallas import tpu as pltpu
from jax.sharding import PartitionSpec as P

MESH = pl.DeviceIdType.MESH
F32 = jnp.float32
BF16 = jnp.bfloat16
I32 = jnp.int32

epsilon = 1e-06
decay_scale = 8.0
D = 2048
COLS = 512
OFFS = (0, -1, 1, 2)


def dot(a, b):
    return jnp.dot(a, b, preferred_element_type=F32)


def dot_nt(a, b):
    return lax.dot_general(a, b, (((1,), (1,)), ((), ())), preferred_element_type=F32)


def iota(shape, dim):
    return lax.broadcasted_iota(I32, shape, dim)


def mask(cond):
    return jnp.where(cond, 1.0, 0.0)


def div6(v):
    return (v * 171) >> 10


def rms_scale(floats, gain):
    scale = lax.rsqrt(jnp.mean(floats * floats, axis=-1, keepdims=True) + epsilon)
    gains = gain[...].astype(F32)
    return jnp.concatenate(
        [floats[:, 128 * k:128 * k + 128] * scale * gains[k:k + 1, :] for k in range(16)], axis=1
    )


def sigmoid(v):
    return 1.0 / (1.0 + jnp.exp(-v))


def neg_expm1(v):
    series = -v * (1.0 + v * (1 / 2) * (1.0 + v * (1 / 3) * (1.0 + v * (1 / 4) * (1.0 + v * (1 / 5)))))
    return jnp.where(v > -0.1, series, 1.0 - jnp.exp(v))


def kernel(
    mix_gain, conv_taps, input_gate, decay_gate, decay_param, ffn_gain, routes, route_weights,
    branch_gate, hidden_h, proj_x_h, proj_y_h, proj_out_h, conv_h, lru_h, eg_h, eu_h, ed_h,
    dg_h, du_h, dd_h,
    new_hidden, new_lru, new_conv,
    hid, px, py, wo, conv, lru, eg, eu, ed, dgu, dd,
    gx, gy, wgu, wd, nrm, bd_in, bd_dec, csum, gout, pp, rsb, smb, sxb, xall, dtok,
    fstack, sel, comb, perm, qmat, disp, arr, xrows, inner, pe, er, ret, back,
    dhid, dpart, drecv, dsb, dxb,
    lsem, ag_s, ag_r, dw_s, dw_r, rs_s, rs_r, xa_s, xa_r, sm_s, sm_r, da_s, da_r,
    di_s, di_r, er_s, er_r, re_s, re_r, dr_s, dr_r, dx_s, dx_r,
):
    ep = lax.axis_index("ep")
    x = lax.axis_index("tp")
    c = lax.rem(ep, 2)
    chip = lax.div(ep, 2)
    y = lax.rem(chip, 4)
    z = lax.div(chip, 4)

    def m4(v):
        return lax.rem(v + 8, 4)

    def cp(src, dst, ssem, rsem, dev):
        return pltpu.make_async_remote_copy(
            src_ref=src, dst_ref=dst, send_sem=ssem, recv_sem=rsem, device_id=dev, device_id_type=MESH
        )

    scopes = []

    def phase(name):
        if scopes:
            scopes.pop().__exit__(None, None, None)
        if name:
            scopes.append(jax.named_scope(name))
            scopes[-1].__enter__()

    loads = [
        (proj_x_h, px), (proj_y_h, py), (hidden_h, hid), (dg_h, dgu.at[0]), (du_h, dgu.at[1]), (dd_h, dd),
        (conv_h, conv), (lru_h, lru), (proj_out_h, wo), (eg_h.at[0], eg), (eu_h.at[0], eu),
        (ed_h.at[0], ed),
    ]

    def load(k):
        return pltpu.make_async_copy(loads[k][0], loads[k][1], lsem.at[k])

    phase("barrier")
    for k in range(len(loads)):
        load(k).start()

    bar = pltpu.get_barrier_semaphore()

    def greet(k, carry):
        pl.semaphore_signal(bar, inc=1, device_id=(lax.rem(ep + k, 32), x), device_id_type=MESH)
        return carry

    lax.fori_loop(1, 32, greet, 0)
    for k in (1, 2, 3):
        pl.semaphore_signal(bar, inc=1, device_id=(ep, m4(x + k)), device_id_type=MESH)
    load(0).wait()
    load(1).wait()
    pl.semaphore_wait(bar, 34)

    phase("ag_start")
    own = (px, py)
    bufs = (gx, gy)
    first = (y, z)
    second = (z, y)

    def chip_of(h, f, s):
        return (s * 4 + f) if h == 0 else (f * 4 + s)

    def slot(h, f, s, cc):
        return bufs[h].at[s, f, cc] if h == 0 else bufs[h].at[f, s, cc]

    def piece(h, f, s, half):
        return slot(h, f, s, c).at[pl.ds(32 * half, 32), :]

    def dev(h, f, s, cc):
        return (chip_of(h, f, s) * 2 + cc, x)

    sent = []

    def go(copy):
        copy.start()
        sent.append(copy)

    def to_f(h, step, idx, src, dst):
        go(cp(src, dst, ag_s.at[h, idx], ag_r.at[h, idx], dev(h, m4(first[h] + step), second[h], c)))

    def to_s(h, step, idx, src, dst):
        go(cp(src, dst, ag_s.at[h, idx], ag_r.at[h, idx], dev(h, first[h], m4(second[h] + step), c)))

    def to_p(h, idx, src, dst):
        go(cp(src, dst, ag_s.at[h, idx], ag_r.at[h, idx], (chip * 2 + 1 - c, x)))

    def got(h, idx, dst):
        cp(dst, dst, ag_s.at[h, idx], ag_r.at[h, idx], (chip * 2 + 1 - c, x)).wait_recv()

    def second_phase(h, i, src):
        f, s = m4(first[h] + OFFS[i]), second[h]
        to_s(h, 1, 4 + 4 * i, src, slot(h, f, s, c))
        to_s(h, -1, 5 + 4 * i, src, slot(h, f, s, c))

    def across(h, i, si, src=None):
        f, s = m4(first[h] + OFFS[i]), m4(second[h] + OFFS[si])
        mine = slot(h, f, s, c)
        to_p(h, 20 + 4 * si + i, mine if src is None else src, mine)

    for h in range(2):
        f, s = first[h], second[h]
        to_f(h, 1, 0, own[h], slot(h, f, s, c))
        to_f(h, -1, 1, own[h], slot(h, f, s, c))
    for h in range(2):
        second_phase(h, 0, own[h])
        across(h, 0, 0, own[h])
    gx[z, y, c] = px[...]
    gy[z, y, c] = py[...]

    r64 = iota((64, 128), 0)
    c128 = iota((64, 128), 1)
    put = (mask(c128 == r64).astype(BF16), mask(c128 == r64 + 64).astype(BF16))

    phase("dense_w_start")
    load(3).wait()
    load(4).wait()
    load(5).wait()
    wsrc = (dgu, dd)
    wdst = (wgu, wd)

    def w_go(a, idx, src, dst, device):
        go(cp(src, dst, dw_s.at[a, idx], dw_r.at[a, idx], device))

    def w_got(a, idx, dst):
        cp(dst, dst, dw_s.at[a, idx], dw_r.at[a, idx], (chip * 2 + 1 - c, x)).wait_recv()

    for a in range(2):
        w_go(a, 0, wsrc[a], wdst[a].at[c, x], (ep, m4(x + 1)))
        w_go(a, 1, wsrc[a], wdst[a].at[c, x], (ep, m4(x - 1)))
        w_go(a, 4, wsrc[a], wdst[a].at[c, x], (chip * 2 + 1 - c, x))
    wgu[c, x] = dgu[...]
    wd[c, x] = dd[...]

    def w_half(a, xx, half):
        if a == 0:
            return wgu.at[c, xx, half]
        return wd.at[c, xx, pl.ds(96 * half, 96), :]

    phase("norm")
    load(2).wait()
    nrm[...] = rms_scale(hid[...].astype(F32), mix_gain).astype(BF16)

    phase("ag_first")
    for h in range(2):
        f, s = first[h], second[h]
        lo, hi = m4(f - 1), m4(f + 1)
        got(h, 0, slot(h, lo, s, c))
        to_f(h, 1, 2, piece(h, lo, s, 0), piece(h, lo, s, 0))
        second_phase(h, 1, slot(h, lo, s, c))
        across(h, 1, 0)
        got(h, 1, slot(h, hi, s, c))
        to_f(h, -1, 3, piece(h, hi, s, 1), piece(h, hi, s, 1))
        second_phase(h, 2, slot(h, hi, s, c))
        across(h, 2, 0)

    def arrivals(h, i):
        f, s = m4(first[h] + OFFS[i]), second[h]
        lo, hi = m4(s - 1), m4(s + 1)
        got(h, 4 + 4 * i, slot(h, f, lo, c))
        to_s(h, 1, 6 + 4 * i, piece(h, f, lo, 0), piece(h, f, lo, 0))
        across(h, i, 1)
        got(h, 5 + 4 * i, slot(h, f, hi, c))
        to_s(h, -1, 7 + 4 * i, piece(h, f, hi, 1), piece(h, f, hi, 1))
        across(h, i, 2)

    def last(h, i):
        f, s = m4(first[h] + OFFS[i]), m4(second[h] + 2)
        got(h, 6 + 4 * i, piece(h, f, s, 0))
        got(h, 7 + 4 * i, piece(h, f, s, 1))
        across(h, i, 3)

    phase("routes")
    e32 = iota((32, 64), 0)
    oh = [mask(routes[r:r + 1, :] == e32) for r in range(2)]
    both = oh[0] + oh[1]
    upper = mask(iota((64, 64), 0) < iota((64, 64), 1)).astype(BF16)
    rank1 = (both * (dot(both.astype(BF16), upper) + 1.0)).astype(BF16)
    eye = mask(iota((64, 64), 0) == iota((64, 64), 1)).astype(BF16)

    phase("ag_a0")
    for h in range(2):
        arrivals(h, 0)
    for h in range(2):
        f, s = m4(first[h] + 2), second[h]
        got(h, 2, piece(h, f, s, 0))
        got(h, 3, piece(h, f, s, 1))
        second_phase(h, 3, slot(h, f, s, c))
        across(h, 3, 0)

    phase("blockdiag")
    for p in range(4):
        for gate, block in ((input_gate, bd_in), (decay_gate, bd_dec)):
            for k in range(2):
                block[p, 64 * k:64 * k + 64, :] = dot(gate[2 * p + k], put[k]).astype(BF16)

    phase("ag_a1")
    for h in range(2):
        arrivals(h, 1)

    phase("conv")
    load(6).wait()
    taps = conv_taps[...].astype(F32)
    csum[...] = sum(conv[k].astype(F32) * taps[k:k + 1, :] for k in range(3))
    new_conv[0] = conv[1]
    new_conv[1] = conv[2]

    phase("ag_a2")
    for h in range(2):
        arrivals(h, 2)

    phase("selmat")
    tt = mask((iota((64, 512), 1) & 63) == iota((64, 512), 0)).astype(BF16)
    spread = dot(rank1, tt).astype(BF16)
    rows = iota((1536, 32), 0)
    ecol = iota((1536, 32), 1) * 48
    erow = mask((rows >= ecol) & (rows < ecol + 48)).astype(BF16)
    row1 = iota((1536, 1), 0)
    six1 = div6(row1 >> 3)
    rin = row1 - six1 * 48
    ck1 = div6(rin)
    slot1 = (rin - 6 * ck1 + 1).astype(F32)
    ckcol = iota((1536, 512), 1) >> 6
    sel[...] = mask((dot(erow, spread) == slot1) & (ck1 == ckcol)).astype(BF16)

    phase("ag_l0")
    for h in range(2):
        last(h, 0)
    for h in range(2):
        arrivals(h, 3)

    phase("perms")
    pr = iota((384, 384), 0)
    pc = iota((384, 384), 1)
    prc = div6(pr >> 3)
    prr = pr - 48 * prc
    prs = div6(prr)
    perm[...] = mask(pc == prs * 48 + prc * 6 + (prr - 6 * prs)).astype(BF16)
    qr = iota((512, 384), 0)
    qc = iota((512, 384), 1)
    qslot = qr & 7
    qmat[...] = mask((qslot < 6) & (qc == ((qr >> 3) & 1) * 192 + (qr >> 4) * 6 + qslot)).astype(BF16)

    phase("ag_l1")
    for h in range(2):
        last(h, 1)

    phase("combs")
    wfull = route_weights[0:1, :] * oh[0] + route_weights[1:2, :] * oh[1]
    whi = wfull.astype(BF16)
    wlo = (wfull - whi.astype(F32)).astype(BF16)
    expand = mask((iota((32, 512), 1) >> 4) == iota((32, 512), 0)).astype(BF16)
    ccol = iota((64, 512), 1)
    hit = dot(dot_nt(eye, rank1).astype(BF16), expand) == ((ccol & 7) + 1).astype(F32)
    ehi = dot(dot_nt(eye, whi).astype(BF16), expand)
    elo = dot(dot_nt(eye, wlo).astype(BF16), expand)
    for j in range(2):
        here = hit & (((ccol >> 3) & 1) == j)
        comb[j, 0] = jnp.where(here, ehi, 0.0).astype(BF16)
        comb[j, 1] = jnp.where(here, elo, 0.0).astype(BF16)

    phase("ag_l2")
    for h in range(2):
        last(h, 2)
    for h in range(2):
        last(h, 3)

    phase("ag_partner")
    for h in range(2):
        for si in range(4):
            for i in range(4):
                f, s = m4(first[h] + OFFS[i]), m4(second[h] + OFFS[si])
                got(h, 20 + 4 * si + i, slot(h, f, s, 1 - c))

    phase("proj_lru")
    x_total = dot(nrm[:, 0:512], gx[0].reshape(512, 512))
    y_total = dot(nrm[:, 0:512], gy[0].reshape(512, 512))
    for k in range(1, 4):
        x_total += dot(nrm[:, 512 * k:512 * k + 512], gx[k].reshape(512, 512))
        y_total += dot(nrm[:, 512 * k:512 * k + 512], gy[k].reshape(512, 512))
    x_proj = x_total.astype(BF16)
    new_conv[2] = x_proj
    conv_out = (csum[...] + x_proj.astype(F32) * taps[3:4, :]).astype(BF16)
    load(7).wait()
    for p in range(4):
        lanes = slice(128 * p, 128 * p + 128)
        co = conv_out[:, lanes]
        gate_in = sigmoid(dot(co, bd_in[p]))
        gate_dec = sigmoid(dot(co, bd_dec[p]))
        log_sig = -jnp.log(1.0 + jnp.exp(-decay_param[:, lanes]))
        log_decay = decay_scale * gate_dec * log_sig
        inject = jnp.sqrt(neg_expm1(2.0 * log_decay))
        state = jnp.exp(log_decay) * lru[:, lanes] + inject * gate_in * co.astype(F32)
        new_lru[:, lanes] = state
        yv = y_total[:, lanes].astype(BF16).astype(F32)
        gout[:, lanes] = (state * jax.nn.gelu(yv, approximate=True)).astype(BF16)

    phase("outproj")
    load(8).wait()
    for k in range(4):
        lanes = slice(512 * k, 512 * k + 512)
        pp[:, :, lanes] = dot(gout[...], wo[:, lanes]).reshape(4, 16, 512).astype(BF16)

    def rs(k):
        to = m4(x + k)
        return cp(pp.at[to], rsb.at[x], rs_s.at[k], rs_r.at[k], (ep, to))

    for k in (2, 1, 3):
        go(rs(k))

    phase("dense_w_relay")
    for a in range(2):
        lo, hi = m4(x - 1), m4(x + 1)
        w_got(a, 0, wdst[a].at[c, lo])
        part = w_half(a, lo, 0)
        w_go(a, 2, part, part, (ep, hi))
        w_go(a, 5, wdst[a].at[c, lo], wdst[a].at[c, lo], (chip * 2 + 1 - c, x))
        w_got(a, 1, wdst[a].at[c, hi])
        part = w_half(a, hi, 1)
        w_go(a, 3, part, part, (ep, lo))
        w_go(a, 6, wdst[a].at[c, hi], wdst[a].at[c, hi], (chip * 2 + 1 - c, x))

    phase("rs_wait")
    mixed = pp[x].astype(F32)
    for k in (1, 3, 2):
        frm = m4(x - k)
        cp(rsb.at[frm], rsb.at[frm], rs_s.at[k], rs_r.at[k], (ep, frm)).wait_recv()
        mixed += rsb[frm].astype(F32)
    summed = (hid[pl.ds(pl.multiple_of(16 * x, 16), 16), :].astype(F32) + mixed).astype(BF16)
    for k in range(4):
        smb[k] = summed[:, 512 * k:512 * k + 512]
    xall[x] = rms_scale(summed.astype(F32), ffn_gain).astype(BF16)
    dtok[chip] = xall[x]

    phase("ffn_send")
    for k in (2, 1, 3):
        to = m4(x + k)
        go(cp(xall.at[x], xall.at[x], xa_s.at[k], xa_r.at[k], (ep, to)))

    def tok(k):
        to = lax.rem(chip + k, 16)
        return cp(xall.at[x], dtok.at[chip], da_s.at[k], da_r.at[k], (to * 2 + c, x))

    def each(first_k, end_k, act):
        def step(k, carry):
            act(k)
            return carry
        lax.fori_loop(first_k, end_k, step, 0)

    each(1, 16, lambda k: tok(k).start())
    for k in (2, 1, 3):
        to = m4(x + k)
        go(cp(smb.at[to], sxb.at[x], sm_s.at[k], sm_r.at[k], (ep, to)))
    sxb[x] = smb[x]

    phase("xag_wait")
    for k in (1, 3, 2):
        frm = m4(x - k)
        cp(xall.at[frm], xall.at[frm], xa_s.at[k], xa_r.at[k], (ep, frm)).wait_recv()
    phase("dispatch")
    for k in range(8):
        fstack[64 * k:64 * k + 64, :] = xall[:, :, 256 * k:256 * k + 256].reshape(64, 256)
    for k in range(4):
        part = slice(384 * k, 384 * k + 384)
        disp[8 * k:8 * k + 8] = dot(sel[part, :], fstack[...]).reshape(8, 48, 256).astype(BF16)
    arr[ep] = disp[ep]

    def route(k):
        to = lax.rem(ep + k, 32)
        return cp(disp.at[to], arr.at[ep], di_s.at[k], di_r.at[k], (to, x))

    each(1, 32, lambda k: route(k).start())

    phase("dense_w_wait")
    for a in range(2):
        far = m4(x + 2)
        w_got(a, 2, w_half(a, far, 0))
        w_got(a, 3, w_half(a, far, 1))
        w_go(a, 7, wdst[a].at[c, far], wdst[a].at[c, far], (chip * 2 + 1 - c, x))
    for a in range(2):
        for idx, off in ((4, 0), (5, -1), (6, 1), (7, 2)):
            w_got(a, idx, wdst[a].at[1 - c, m4(x + off)])

    def tok_got(k):
        frm = lax.rem(chip + 16 - k, 16)
        cp(dtok.at[frm], dtok.at[frm], da_s.at[k], da_r.at[k], (frm * 2 + c, x)).wait_recv()

    phase("dense_tok_wait")
    each(1, 16, tok_got)
    phase("dense_gu")
    for cc in range(2):
        gv = jnp.zeros((256, 192), F32)
        uv = jnp.zeros((256, 192), F32)
        for k in range(4):
            part = dtok[:, :, 512 * k:512 * k + 512].reshape(256, 512)
            gv += dot_nt(part, wgu[cc, k, 0])
            uv += dot_nt(part, wgu[cc, k, 1])
        dhid[cc] = (gv * sigmoid(gv) * uv).astype(BF16)
    phase("dense_down")
    for k in range(4):
        out = dot(dhid[0], wd[0, k]) + dot(dhid[1], wd[1, k])
        dpart[:, :, 512 * k:512 * k + 512] = out.reshape(16, 16, 512).astype(BF16)

    def dred(k):
        to = lax.rem(chip + k, 16)
        return cp(dpart.at[to], drecv.at[chip], dr_s.at[k], dr_r.at[k], (to * 2 + c, x))

    each(1, 16, lambda k: dred(k).start())
    drecv[chip] = dpart[chip]

    def route_got(k):
        frm = lax.rem(ep + 32 - k, 32)
        cp(arr.at[frm], arr.at[frm], di_s.at[k], di_r.at[k], (frm, x)).wait_recv()

    phase("dispatch_wait")
    each(1, 32, route_got)
    phase("perm_rows")
    for k in range(4):
        moved = dot(perm[...], arr[8 * k:8 * k + 8].reshape(384, 256)).astype(BF16)
        for j in range(8):
            xrows[48 * k:48 * k + 48, 256 * j:256 * j + 256] = moved[48 * j:48 * j + 48, :]
    phase("expert_gu")
    load(9).wait()
    load(10).wait()
    for k in range(3):
        lanes = slice(256 * k, 256 * k + 256)
        gv = dot(xrows[...], eg[:, lanes])
        uv = dot(xrows[...], eu[:, lanes])
        inner[:, lanes] = (gv * sigmoid(gv) * uv).astype(BF16)
    phase("expert_down")
    load(11).wait()
    for k in (2, 1, 3, 0):
        to = m4(x + k)
        pe[to] = dot(inner[...], ed[:, pl.ds(pl.multiple_of(512 * to, 512), 512)]).astype(BF16)
        if k:
            go(cp(pe.at[to], er.at[x], er_s.at[k], er_r.at[k], (ep, to)))

    def dred_got(k):
        frm = lax.rem(chip + 16 - k, 16)
        cp(drecv.at[frm], drecv.at[frm], dr_s.at[k], dr_r.at[k], (frm * 2 + c, x)).wait_recv()

    phase("dense_red_wait")
    each(1, 16, dred_got)
    phase("dense_sum")
    for k in range(4):
        dsb[k] = jnp.sum(drecv[:, :, 512 * k:512 * k + 512].astype(F32), axis=0).astype(BF16)
    for k in (2, 1, 3):
        to = m4(x + k)
        go(cp(dsb.at[to], dxb.at[x], dx_s.at[k], dx_r.at[k], (ep, to)))
    dxb[x] = dsb[x]

    phase("er_wait")
    total = pe[x].astype(F32)
    for k in (1, 3, 2):
        frm = m4(x - k)
        cp(er.at[frm], er.at[frm], er_s.at[k], er_r.at[k], (ep, frm)).wait_recv()
        total += er[frm].astype(F32)
    phase("ret_build")
    total = total.astype(BF16)
    ret[...] = (
        dot(qmat[:, 0:192], total[:, 0:256]) + dot(qmat[:, 192:384], total[:, 256:512])
    ).reshape(32, 16, 256).astype(BF16)
    back[ep] = ret[ep]

    def giveback(k):
        to = lax.rem(ep + k, 32)
        return cp(ret.at[to], back.at[ep], re_s.at[k], re_r.at[k], (to, x))

    each(1, 32, lambda k: giveback(k).start())

    phase("rest_wait")
    for k in (1, 3, 2):
        frm = m4(x - k)
        cp(sxb.at[frm], sxb.at[frm], sm_s.at[k], sm_r.at[k], (ep, frm)).wait_recv()
        cp(dxb.at[frm], dxb.at[frm], dx_s.at[k], dx_r.at[k], (ep, frm)).wait_recv()
    phase("rest")
    share = sigmoid(branch_gate[...])
    rest = sxb[...].reshape(64, 512).astype(F32) + share * dxb[...].reshape(64, 512).astype(F32)

    def back_got(k):
        frm = lax.rem(ep + 32 - k, 32)
        cp(back.at[frm], back.at[frm], re_s.at[k], re_r.at[k], (frm, x)).wait_recv()

    phase("back_wait")
    each(1, 32, back_got)
    phase("combine")
    rows_back = back[...].reshape(512, 256)
    for j in range(2):
        lanes = slice(256 * j, 256 * j + 256)
        esum = dot(comb[j, 0], rows_back) + dot(comb[j, 1], rows_back)
        new_hidden[:, lanes] = (rest[:, lanes] + esum).astype(BF16)

    phase("send_wait")
    for copy in sent:
        copy.wait_send()
    each(1, 16, lambda k: tok(k).wait_send())
    each(1, 16, lambda k: dred(k).wait_send())
    each(1, 32, lambda k: route(k).wait_send())
    each(1, 32, lambda k: giveback(k).wait_send())
    phase(None)


def publish(a, b, c, a_out, b_out, c_out):
    a_out[...] = a[...]
    b_out[...] = b[...]
    c_out[...] = c[...]


def on_device(
    hidden, mix_gain, proj_x, proj_y, conv_taps, input_gate, decay_gate, decay_param, proj_out,
    conv_state, lru_state, ffn_gain, routes, route_weights, expert_gate, expert_up, expert_down,
    dense_gate, dense_up, dense_down, branch_gate,
):
    vmem = pl.BlockSpec(memory_space=pltpu.VMEM)
    hbm = pl.BlockSpec(memory_space=pl.ANY)
    V = pltpu.VMEM
    dma = pltpu.SemaphoreType.DMA
    scratch = [
        V((64, D), BF16), V((64, COLS), BF16), V((64, COLS), BF16), V((COLS, D), BF16),
        V((3, 64, COLS), BF16), V((64, COLS), F32), V((D, 768), BF16), V((D, 768), BF16),
        V((768, D), BF16), V((2, 192, COLS), BF16), V((192, COLS), BF16),
        V((4, 4, 2, 64, COLS), BF16), V((4, 4, 2, 64, COLS), BF16),
        V((2, 4, 2, 192, COLS), BF16), V((2, 4, 192, COLS), BF16), V((64, D), BF16),
        V((4, 128, 128), BF16), V((4, 128, 128), BF16), V((64, COLS), F32), V((64, COLS), BF16),
        V((4, 16, D), BF16), V((4, 16, D), BF16), V((4, 16, COLS), BF16), V((4, 16, COLS), BF16),
        V((4, 16, D), BF16), V((16, 16, D), BF16),
        V((512, 256), BF16), V((1536, 512), BF16), V((2, 2, 64, 512), BF16), V((384, 384), BF16),
        V((512, 384), BF16), V((32, 48, 256), BF16), V((32, 48, 256), BF16), V((192, D), BF16),
        V((192, 768), BF16), V((4, 192, COLS), BF16), V((4, 192, COLS), BF16),
        V((32, 16, 256), BF16), V((32, 16, 256), BF16),
        V((2, 256, 192), BF16), V((16, 16, D), BF16), V((16, 16, D), BF16),
        V((4, 16, COLS), BF16), V((4, 16, COLS), BF16),
        dma((12,)), dma((2, 36)), dma((2, 36)), dma((2, 8)), dma((2, 8)), dma((4,)), dma((4,)),
        dma((4,)), dma((4,)), dma((4,)), dma((4,)), dma((16,)), dma((16,)), dma((32,)), dma((32,)),
        dma((4,)), dma((4,)), dma((32,)), dma((32,)), dma((16,)), dma((16,)), dma((4,)), dma((4,)),
    ]
    shapes = (
        jax.ShapeDtypeStruct((64, COLS), BF16),
        jax.ShapeDtypeStruct((64, COLS), F32),
        jax.ShapeDtypeStruct((3, 64, COLS), BF16),
    )
    outs = pl.pallas_call(
        kernel,
        out_shape=shapes,
        in_specs=[vmem] * 9 + [hbm] * 12,
        out_specs=(vmem, vmem, vmem),
        scratch_shapes=scratch,
        compiler_params=pltpu.CompilerParams(
            collective_id=0, has_side_effects=True, vmem_limit_bytes=58 * 1024 * 1024
        ),
        name="decode_layer",
    )(
        mix_gain.reshape(16, 128), conv_taps, input_gate, decay_gate, decay_param.reshape(1, COLS),
        ffn_gain.reshape(16, 128), routes.T, route_weights.T, branch_gate.reshape(1, COLS),
        hidden, proj_x, proj_y, proj_out, conv_state.transpose(1, 0, 2), lru_state, expert_gate, expert_up,
        expert_down, dense_gate.T, dense_up.T, dense_down,
    )
    new_hidden, new_lru, new_conv = pl.pallas_call(
        publish,
        out_shape=shapes,
        in_specs=[vmem] * 3,
        out_specs=(vmem,) * 3,
        name="publish",
    )(*outs)
    return (new_hidden, new_lru, new_conv.transpose(1, 0, 2))


def solution(mesh):
    in_specs = (
        P("ep", None), P(), P("ep", "tp"), P("ep", "tp"), P(None, "tp"), P("tp", None, None),
        P("tp", None, None), P("tp"), P("tp", None), P("ep", None, "tp"), P("ep", "tp"), P(),
        P("ep", None), P("ep", None), P("ep", None, "tp"), P("ep", None, "tp"),
        P("ep", "tp", None), P("tp", "ep"), P("tp", "ep"), P("ep", "tp"), P("tp"),
    )
    out_specs = (P("ep", "tp"), P("ep", "tp"), P("ep", None, "tp"))
    return jax.shard_map(
        on_device, mesh=mesh, in_specs=in_specs, out_specs=out_specs, check_vma=False
    )
```
